32 devices in a mesh: ep: 16 (over z, y, x), tp: 2 (over core).
Axes of the slice: x: 2, y: 2, z: 4, core: 2. Of those that a mesh axis runs over, the one named last changes fastest.
Arguments:
- tokens: bfloat16 [384, 2048], P('ep'), may hold values from -6 to 6
- norm_gain: bfloat16 [2048], replicated, may hold values from 0.099609375 to 1.8984375
- query_w: bfloat16 [2048, 1024], P(None, 'tp'), may hold values from -0.125 to 0.125
- key_w: bfloat16 [2048, 128], replicated, may hold values from -0.125 to 0.125
- value_w: bfloat16 [2048, 128], replicated, may hold values from -0.125 to 0.125
- forget_w: bfloat16 [2048, 16], replicated, may hold values from -0.125 to 0.125
- forget_bias: float32 [16], replicated, may hold values from 0 to 4
- query_gain: bfloat16 [64], replicated, may hold values from 0.099609375 to 1.8984375
- key_gain: bfloat16 [64], replicated, may hold values from 0.099609375 to 1.8984375
- cache_key: bfloat16 [384, 2, 64, 1024], P('ep', 'tp'), may hold values from -6 to 6
- cache_value: bfloat16 [384, 2, 64, 1024], P('ep', 'tp'), may hold values from -6 to 6
- cache_gate: float32 [384, 16, 1024], P('ep', 'tp'), may hold values from -105 to 0, as said below
- cache_len: int32 [384], P('ep'), may hold values from 256 to 1024
- out_w: bfloat16 [1024, 2048], P('tp'), may hold values from -0.1875 to 0.1875
- post_gain: bfloat16 [2048], replicated, may hold values from 0.099609375 to 1.8984375
- branch_gate: bfloat16 [2048], replicated, may hold values from -0.125 to 0.125
- dense_gate_w: bfloat16 [2048, 16384], P(None, ('ep', 'tp')), may hold values from -0.125 to 0.125
- dense_up_w: bfloat16 [2048, 16384], P(None, ('ep', 'tp')), may hold values from -1.3258252 to 1.3258252
- dense_down_w: bfloat16 [16384, 2048], P(('ep', 'tp')), may hold values from -0.046875 to 0.046875
- expert_choice: int32 [384, 2], P('ep'), may hold values from 0 to 15, as said below
- route_weight: float32 [384, 2], P('ep'), may hold values from 0.1 to 1
- expert_gate_w: bfloat16 [16, 2048, 1024], P('ep', None, 'tp'), may hold values from -0.125 to 0.125
- expert_up_w: bfloat16 [16, 2048, 1024], P('ep', None, 'tp'), may hold values from -0.125 to 0.125
- expert_down_w: bfloat16 [16, 1024, 2048], P('ep', 'tp'), may hold values from -0.1875 to 0.1875
Outputs:
- mixed_out: bfloat16 [384, 2048], P('ep', 'tp')
- fresh_key: bfloat16 [384, 2, 64], P('ep', 'tp')
- fresh_value: bfloat16 [384, 2, 64], P('ep', 'tp')
- fresh_gate: float32 [384, 16], P('ep', 'tp')
The draws below stay inside these ranges and needn't reach their ends.
Inputs may be any that keep to these rules, and one draw needn't show every extreme that they name: `cache_gate`: Non-increasing along positions. `expert_choice`: experts 4 * g to 4 * g + 3 form group g. A token names 2 different experts of one group. Among the 24 tokens of one index of ep, those at even offsets all choose one group and the others choose other groups; no expert is named more than 6 times by them, and some expert exactly 6 times.
All inputs are finite; a program needn't handle non-finite values.
Results may differ from the reference program's by a relative error of at most 0.014.
Values may be sent and summed in bfloat16 or wider, within the bound.
A program may use at most 128 MiB of HBM per device.

```python
import math
import jax
import jax.numpy as jnp
from jax import lax

D = 2048
HEADS = 16
KV = 2
HD = 64
FFE = 1024
FF2 = 16384
GROUPS = 4
TOPK = 2
SEQ_DEV = 24
STORED_SLOTS = 1024
BATCH_ENTRIES = 384
EXPERTS = 16
EPG = 4
CAP = 6
N_EP = 16
N_TP = 2


def draw_cache_gate(key, part):
    derived_prng_seeds = jax.random.split(jax.random.fold_in(key, 11), 7)
    fast_share = 0.5
    is_fast = jax.random.uniform(derived_prng_seeds[0], (HEADS,)) < fast_share
    slow_rate = jax.random.uniform(derived_prng_seeds[1], (HEADS,), minval=0.3, maxval=0.8) / STORED_SLOTS
    fast_rate = 1.0 / jax.random.uniform(derived_prng_seeds[2], (HEADS,), minval=30.0, maxval=100.0)
    per_attender_fading = jnp.where(is_fast, fast_rate, slow_rate)
    batch_multiplier = jnp.exp(jax.random.uniform(derived_prng_seeds[3], (BATCH_ENTRIES, 1, 1), minval=math.log(0.6), maxval=math.log(1.6)))
    outer_level_logits = jax.random.uniform(derived_prng_seeds[4], (BATCH_ENTRIES, HEADS, STORED_SLOTS), minval=0.5, maxval=1.5)
    contiguous_first_slot = jax.random.randint(derived_prng_seeds[5], (BATCH_ENTRIES, 3), 0, STORED_SLOTS)
    contiguous_span = jax.random.uniform(derived_prng_seeds[6], (BATCH_ENTRIES, 3), minval=0.22, maxval=0.69)
    current_slot_offset = jnp.arange(STORED_SLOTS)[None, None, :]
    contiguous_tiles = jnp.sum(jnp.where(current_slot_offset == contiguous_first_slot[:, :, None], contiguous_span[:, :, None], 0.0), axis=1)
    increment_fading_exponent = -(per_attender_fading[None, :, None] * batch_multiplier * outer_level_logits) - contiguous_tiles[:, None, :]
    return jnp.cumsum(increment_fading_exponent, axis=2).astype(jnp.float32)


def draw_dense_up_w(key, part):
    base_key = jax.random.fold_in(key, 21)
    column = jnp.arange(FF2, dtype=jnp.float32) / FF2
    entries = jnp.clip(jax.random.normal(base_key, (D, FF2)), -6.0, 6.0)
    column_scale = jnp.exp(math.log(10.0) * column)
    return (entries * column_scale[None, :] * D ** (-0.5)).astype(jnp.bfloat16)


def draw_expert_choice(key, part):
    derived_prng_seeds = jax.random.split(jax.random.fold_in(key, 31), 3)
    blocks = BATCH_ENTRIES // SEQ_DEV
    even_group = jax.random.randint(derived_prng_seeds[0], (blocks, 1), 0, GROUPS)
    other_group = (even_group + 1 + jax.random.randint(derived_prng_seeds[1], (blocks, SEQ_DEV), 0, GROUPS - 1)) % GROUPS
    offset = jnp.arange(SEQ_DEV)[None, :]
    group_id = jnp.where(offset % 2 == 0, even_group, other_group)
    member_of = (group_id[:, :, None] == jnp.arange(GROUPS)[None, None, :]).astype(jnp.int32)
    rank_in = jnp.sum((jnp.cumsum(member_of, axis=1) - member_of) * member_of, axis=2)
    shift_by = jax.random.randint(derived_prng_seeds[2], (blocks, GROUPS), 0, EPG)
    start_at = jnp.sum(member_of * shift_by[:, None, :], axis=2)
    first_member = (start_at + rank_in) % EPG
    second = (first_member + 1) % EPG
    chosen = jnp.stack([group_id * EPG + first_member, group_id * EPG + second], axis=-1)
    return chosen.reshape(BATCH_ENTRIES, TOPK).astype(jnp.int32)


def place_ends(values, stream_key, least, high):
    dims = values.shape
    spot = [jax.random.randint(jax.random.fold_in(stream_key, axis), (), 0, dims[axis]) for axis in range(len(dims))]
    values = values.at[tuple(spot)].set(least)
    longest = dims.index(max(dims))
    spot[longest] = (spot[longest] + 1) % dims[longest]
    return values.at[tuple(spot)].set(high)


def levels(own_key, dims, cuts, smallest, top_value):
    level, own = 1.0, jax.random.fold_in(own_key, 6)
    for axis_at, blocks in cuts:
        steps = jnp.exp(jax.random.uniform(jax.random.fold_in(own, axis_at), (blocks,), jnp.float32, smallest / len(cuts), top_value / len(cuts)))
        level = level * jnp.repeat(steps, dims[axis_at] // blocks).reshape([-1 if axis == axis_at else 1 for axis in range(len(dims))])
    return level


def bell_draw(key, dims, scale, reach, pieces=(), held_as=jnp.bfloat16):
    values = scale * jax.random.normal(key, dims, jnp.float32)
    if pieces:
        values = values * levels(key, dims, pieces, -0.22, 0.18)
    return jnp.clip(values, -reach, reach).astype(held_as)


def setup_inputs(seed: int = 0) -> dict:
    streams_of = jax.random.split(jax.random.key(seed), 25)
    return {
        "tokens": bell_draw(streams_of[0], (BATCH_ENTRIES, D), 1.0, 6.0, ((0, 16),)),
        "norm_gain": jnp.clip(1.0 + 0.18 * jax.random.normal(streams_of[1], (D,), jnp.float32), 0.099609375, 1.8984375).astype(jnp.bfloat16),
        "query_w": bell_draw(streams_of[2], (D, HEADS * HD), D ** -0.5, 0.125, ((1, 2),)),
        "key_w": bell_draw(streams_of[3], (D, KV * HD), D ** -0.5, 0.125),
        "value_w": bell_draw(streams_of[4], (D, KV * HD), D ** -0.5, 0.125),
        "forget_w": bell_draw(streams_of[5], (D, HEADS), D ** -0.5, 0.125),
        "forget_bias": jnp.clip(jax.random.uniform(streams_of[6], (HEADS,), jnp.float32, 0.0, 4.0), 0.0, 4.0),
        "query_gain": jnp.clip(1.0 + 0.18 * jax.random.normal(streams_of[7], (HD,), jnp.float32), 0.099609375, 1.8984375).astype(jnp.bfloat16),
        "key_gain": jnp.clip(1.0 + 0.18 * jax.random.normal(streams_of[8], (HD,), jnp.float32), 0.099609375, 1.8984375).astype(jnp.bfloat16),
        "cache_key": bell_draw(streams_of[9], (BATCH_ENTRIES, KV, HD, STORED_SLOTS), 1.0, 6.0, ((0, 16), (1, 2))),
        "cache_value": bell_draw(streams_of[10], (BATCH_ENTRIES, KV, HD, STORED_SLOTS), 1.0, 6.0, ((0, 16), (1, 2))),
        "cache_gate": draw_cache_gate(jax.random.fold_in(streams_of[24], 71), 0),
        "cache_len": place_ends(jax.random.randint(streams_of[12], (BATCH_ENTRIES,), STORED_SLOTS // 4, STORED_SLOTS + 1), jax.random.fold_in(streams_of[12], 1), STORED_SLOTS // 4, STORED_SLOTS).astype(jnp.int32),
        "out_w": bell_draw(streams_of[13], (HEADS * HD, D), (HEADS * HD) ** -0.5, 0.1875, ((0, 2),)),
        "post_gain": jnp.clip(1.0 + 0.18 * jax.random.normal(streams_of[14], (D,), jnp.float32), 0.099609375, 1.8984375).astype(jnp.bfloat16),
        "branch_gate": bell_draw(streams_of[15], (D,), D ** -0.5, 0.125),
        "dense_gate_w": bell_draw(streams_of[16], (D, FF2), D ** -0.5, 0.125, ((1, 32),)),
        "dense_up_w": draw_dense_up_w(jax.random.fold_in(streams_of[24], 71), 0),
        "dense_down_w": bell_draw(streams_of[18], (FF2, D), FF2 ** -0.5, 0.046875, ((0, 32),)),
        "expert_choice": draw_expert_choice(jax.random.fold_in(streams_of[24], 71), 0),
        "route_weight": jnp.clip(0.1 + 0.9 * jax.random.uniform(streams_of[20], (BATCH_ENTRIES, TOPK), jnp.float32) ** levels(streams_of[20], (BATCH_ENTRIES, TOPK), ((0, 16),), -0.2, 0.2), 0.1, 1.0),
        "expert_gate_w": bell_draw(streams_of[21], (EXPERTS, D, FFE), D ** -0.5, 0.125, ((0, 16), (2, 2))),
        "expert_up_w": bell_draw(streams_of[22], (EXPERTS, D, FFE), D ** -0.5, 0.125, ((0, 16), (2, 2))),
        "expert_down_w": bell_draw(streams_of[23], (EXPERTS, FFE, D), FFE ** -0.5, 0.1875, ((0, 16), (1, 2))),
    }


norm_eps = 1e-06

def rms_scale(values, gain_vec):
    mean_square = lax.optimization_barrier(jnp.mean(values * values, axis=-1, keepdims=True))
    return values * lax.rsqrt(mean_square + norm_eps) * gain_vec

def rounded(values):
    return lax.optimization_barrier(values.astype(jnp.bfloat16)).astype(jnp.float32)

def attend(block_in):
    queries, new_keys, new_values, log_forget, keys_cached, values_cached, gates_cached, lengths = block_in
    row_count = queries.shape[0]
    repeat = HEADS // KV
    score_scale = HD ** (-0.5)
    grouped = queries.reshape(row_count, KV, repeat, HD).astype(jnp.float32)
    scores = jnp.einsum('sgrd,sgdl->sgrl', grouped, keys_cached.astype(jnp.float32)) * score_scale
    own_score = jnp.einsum('sgrd,sgd->sgr', grouped, new_keys.astype(jnp.float32)) * score_scale
    current_slot_offset = lax.broadcasted_iota(jnp.int32, (row_count, STORED_SLOTS), 1)
    at_last = (current_slot_offset == lengths[:, None] - 1)[:, None, :]
    previous = lax.optimization_barrier(jnp.sum(jnp.where(at_last, gates_cached, jnp.zeros_like(gates_cached)), axis=2))
    current = previous + log_forget
    decay_bias = (current[:, :, None] - gates_cached).reshape(row_count, KV, repeat, STORED_SLOTS)
    is_valid = (current_slot_offset < lengths[:, None])[:, None, None, :]
    logits = jnp.where(is_valid, scores + decay_bias, -jnp.inf)
    top_logit = jnp.maximum(lax.optimization_barrier(jnp.max(logits, axis=3)), own_score)
    weights = jnp.exp(logits - top_logit[..., None])
    own_weight = jnp.exp(own_score - top_logit)
    total_weight = lax.optimization_barrier(jnp.sum(weights, axis=3)) + own_weight
    cache_probs = (weights / total_weight[..., None]).astype(jnp.bfloat16)
    own_prob = (own_weight / total_weight).astype(jnp.bfloat16)
    mixed_heads = jnp.einsum('sgrl,sgdl->sgrd', cache_probs.astype(jnp.float32), values_cached.astype(jnp.float32))
    mixed_heads = mixed_heads + own_prob.astype(jnp.float32)[..., None] * new_values.astype(jnp.float32)[:, :, None, :]
    return (mixed_heads.reshape(row_count, HEADS * HD).astype(jnp.bfloat16), current)

def reference(tokens, norm_gain, query_w, key_w, value_w, forget_w, forget_bias, query_gain, key_gain, cache_key, cache_value, cache_gate, cache_len, out_w, post_gain, branch_gate, dense_gate_w, dense_up_w, dense_down_w, expert_choice, route_weight, expert_gate_w, expert_up_w, expert_down_w):
    token_count = tokens.shape[0]
    resid_in = tokens.astype(jnp.float32)
    normed = rms_scale(resid_in, norm_gain.astype(jnp.float32)).astype(jnp.bfloat16)
    queries = jnp.dot(normed, query_w, preferred_element_type=jnp.float32).reshape(token_count, HEADS, HD)
    queries = rms_scale(queries, query_gain.astype(jnp.float32)).astype(jnp.bfloat16)
    fresh_key = jnp.dot(normed, key_w, preferred_element_type=jnp.float32).reshape(token_count, KV, HD)
    fresh_key = rms_scale(fresh_key, key_gain.astype(jnp.float32)).astype(jnp.bfloat16)
    fresh_value = jnp.dot(normed, value_w, preferred_element_type=jnp.float32).astype(jnp.bfloat16).reshape(token_count, KV, HD)
    log_forget = jax.nn.log_sigmoid(jnp.dot(normed, forget_w, preferred_element_type=jnp.float32) + forget_bias)

    def blocks(array_in):
        return array_in.reshape((N_EP, SEQ_DEV) + array_in.shape[1:])
    heads_out, fresh_gate = lax.map(attend, tuple((blocks(array_in) for array_in in (queries, fresh_key, fresh_value, log_forget, cache_key, cache_value, cache_gate, cache_len))))
    heads_out = heads_out.reshape(token_count, HEADS * HD)
    fresh_gate = fresh_gate.reshape(token_count, HEADS)
    head_groups = heads_out.reshape(token_count, N_TP, -1)
    out_parts = out_w.reshape(N_TP, -1, D)
    attn_sum = jnp.zeros((token_count, D), jnp.float32)
    for group_index in range(N_TP):
        attn_sum = attn_sum + rounded(jnp.dot(head_groups[:, group_index], out_parts[group_index], preferred_element_type=jnp.float32))
    resid_out = rounded(resid_in + attn_sum)
    post_norm = rms_scale(resid_out, post_gain.astype(jnp.float32)).astype(jnp.bfloat16)
    branch = jax.nn.sigmoid(jnp.dot(post_norm, branch_gate, preferred_element_type=jnp.float32))
    hidden = jax.nn.silu(jnp.dot(post_norm, dense_gate_w, preferred_element_type=jnp.float32)) * jnp.dot(post_norm, dense_up_w, preferred_element_type=jnp.float32)
    inverse = lax.rsqrt(lax.optimization_barrier(jnp.mean(hidden * hidden, axis=1)) + norm_eps)
    dense_out = rounded(jnp.dot(hidden.astype(jnp.bfloat16), dense_down_w, preferred_element_type=jnp.float32) * inverse[:, None])
    route_total = token_count * TOPK
    route_ids = expert_choice.reshape(-1).astype(jnp.int32)
    limit = N_EP * CAP

    def one_expert(routed_acc, slices):
        gate_mat, up_mat, down_mat, expert_index = slices
        picked = jnp.nonzero(route_ids == expert_index, size=limit, fill_value=route_total)[0].astype(jnp.int32)
        slot_rows = post_norm[jnp.minimum(picked, route_total - 1) // TOPK]
        gate_val = jnp.dot(slot_rows, gate_mat, preferred_element_type=jnp.float32)
        up_val = jnp.dot(slot_rows, up_mat, preferred_element_type=jnp.float32)
        activated = (jax.nn.silu(gate_val) * up_val).astype(jnp.bfloat16)
        act_parts = activated.reshape(limit, N_TP, -1)
        down_parts = down_mat.reshape(N_TP, -1, D)
        expert_out = jnp.zeros((limit, D), jnp.float32)
        for group_index in range(N_TP):
            expert_out = expert_out + rounded(jnp.dot(act_parts[:, group_index], down_parts[group_index], preferred_element_type=jnp.float32))
        routed_acc = routed_acc.at[picked].set(rounded(expert_out), mode='drop')
        return (routed_acc, None)
    routed, _ = lax.scan(one_expert, jnp.zeros((route_total, D), jnp.float32), (expert_gate_w, expert_up_w, expert_down_w, jnp.arange(N_EP, dtype=jnp.int32)))
    expert_sum = lax.optimization_barrier(jnp.sum(route_weight[:, :, None] * routed.reshape(token_count, TOPK, D), axis=1))
    mixed_out = (resid_out + expert_sum + branch[:, None] * dense_out).astype(jnp.bfloat16)
    return (mixed_out, fresh_key, fresh_value, fresh_gate)
```

```python
import functools
import jax
import jax.numpy as jnp
from jax import lax
from jax.experimental import pallas as pl
from jax.experimental.pallas import tpu as pltpu
from jax.sharding import PartitionSpec as P

FF2 = 16384
GROUPS = 4


norm_eps = 1e-06


def rms_scale(values, gain_vec):
    mean_square = jnp.mean(values * values, axis=-1, keepdims=True)
    return values * lax.rsqrt(mean_square + norm_eps) * gain_vec


MESH = pl.DeviceIdType.MESH


def fdot(a, b):
    return jnp.dot(a, b, preferred_element_type=jnp.float32)


def silu(v):
    return v / (1.0 + jnp.exp(-v))


def mlp_kernel(
    ep_count,
    zn,
    capp,
    ff2,
    heads_ref,
    tok_ref,
    gain_ref,
    gate_ref,
    place_ref,
    comb_ref,
    out_hbm,
    dg_hbm,
    du_hbm,
    dd_hbm,
    eg_hbm,
    eu_hbm,
    ed_hbm,
    res_ref,
    wout,
    wg,
    wu,
    wd_own,
    wd_oth,
    xg,
    xu,
    xd_own,
    xd_oth,
    part,
    part_in,
    resid,
    gath,
    hid,
    p_own,
    p_sq,
    p_send,
    p_recv,
    s_send,
    r_recv,
    t_send,
    z_recv,
    rows,
    act,
    e_own,
    e_send,
    e_recv,
    e_out,
    e_ret,
    wsem,
    tp_sem,
    a_send,
    a_recv,
    b_send,
    b_recv,
    f_send,
    f_recv,
    d_sem,
    rs_send,
    rs_recv,
    zs_send,
    zs_recv,
    x_sem,
    er_send,
    er_recv,
):
    pn = ep_count // zn
    me = lax.axis_index("ep")
    c = lax.axis_index("tp")
    z = me // pn
    q = me % pn
    other = 1 - c
    seq, width = tok_ref.shape
    half = width // 2
    full = gath.shape[2]
    fhalf = full // 2
    rows_all = ep_count * seq
    own_cols = pl.ds(pl.multiple_of(c * half, 128), half)
    oth_cols = pl.ds(pl.multiple_of(other * half, 128), half)
    g_cols = pl.ds(pl.multiple_of(c * fhalf, 128), fhalf)

    barrier = pltpu.get_barrier_semaphore()
    for d in range(1, ep_count):
        pl.semaphore_signal(
            barrier, inc=1, device_id=((me + d) % ep_count, c), device_id_type=MESH
        )
    pl.semaphore_signal(barrier, inc=1, device_id=(me, other), device_id_type=MESH)

    loads = [
        (out_hbm, wout),
        (dg_hbm, wg),
        (du_hbm, wu),
        (dd_hbm.at[:, oth_cols], wd_oth),
        (dd_hbm.at[:, own_cols], wd_own),
        (eg_hbm.at[0], xg),
        (eu_hbm.at[0], xu),
        (ed_hbm.at[0, :, oth_cols], xd_oth),
        (ed_hbm.at[0, :, own_cols], xd_own),
    ]
    loads = [pltpu.make_async_copy(a, b, wsem.at[i]) for i, (a, b) in enumerate(loads)]
    for one in loads:
        one.start()

    def remote(src, dst, ssem, rsem, ep_id, tp_id):
        return pltpu.make_async_remote_copy(
            src_ref=src,
            dst_ref=dst,
            send_sem=ssem,
            recv_sem=rsem,
            device_id=(ep_id, tp_id),
            device_id_type=MESH,
        )

    loads[0].wait()
    part[...] = fdot(heads_ref[...], wout[...]).astype(jnp.bfloat16)
    pl.semaphore_wait(barrier, ep_count)
    swap = remote(part, part_in, tp_sem.at[0], tp_sem.at[1], me, other)
    swap.start()
    swap.wait()
    attn = part[...].astype(jnp.float32) + part_in[...].astype(jnp.float32)
    res = (tok_ref[...].astype(jnp.float32) + attn).astype(jnp.bfloat16).astype(jnp.float32)
    resid[...] = res
    post = rms_scale(res, gain_ref[...].astype(jnp.float32)).astype(jnp.bfloat16)
    gath[me, :, :width] = post
    gath[me, :, width:] = place_ref[...]
    branch_in = jnp.sum(
        post.astype(jnp.float32) * gate_ref[...].astype(jnp.float32), axis=1, keepdims=True
    )
    branch = 1.0 / (1.0 + jnp.exp(-branch_in))

    sent = []

    def block_send(o, ssem, rsem, ep_id, tp_id):
        piece = gath.at[o, :, g_cols]
        one = remote(piece, piece, ssem, rsem, ep_id, tp_id)
        one.start()
        sent.append(one)
        return one

    z_sends = []
    for dz in range(1, zn):
        z_sends.append(
            block_send(me, a_send.at[dz], a_recv.at[dz], ((z + dz) % zn) * pn + q, c)
        )
    b_sends = {}
    f_sends = []

    def to_plane(o, dz):
        for dq in range(1, pn):
            b_sends[dz, dq] = block_send(
                o, b_send.at[dz, dq], b_recv.at[dz, dq], z * pn + (q + dq) % pn, c
            )

    to_plane(me, 0)
    for dz in range(1, zn):
        z_sends[dz - 1].wait_recv()
        o = ((z + zn - dz) % zn) * pn + q
        to_plane(o, dz)
        f_sends.append(block_send(o, f_send.at[dz, 0], f_recv.at[dz, 0], me, other))
    for dz in range(zn):
        for dq in range(1, pn):
            b_sends[dz, dq].wait_recv()
            o = ((z + zn - dz) % zn) * pn + (q + pn - dq) % pn
            f_sends.append(block_send(o, f_send.at[dz, dq], f_recv.at[dz, dq], me, other))
    for one in f_sends:
        one.wait_recv()
    for one in sent:
        one.wait_send()

    loads[1].wait()
    loads[2].wait()
    total_sq = jnp.zeros((rows_all, 1), jnp.float32)
    units = wg.shape[1]
    step = min(256, units)
    x = gath[:, :, :width].reshape(rows_all, width)
    for j in range(0, units, step):
        h = silu(fdot(x, wg[:, j : j + step])) * fdot(x, wu[:, j : j + step])
        total_sq = total_sq + jnp.sum(h * h, axis=1, keepdims=True)
        hid[:, j : j + step] = h.astype(jnp.bfloat16)
    lane_sq = jnp.broadcast_to(total_sq, (rows_all, 128)).reshape(ep_count, seq, 128)
    p_sq[...] = lane_sq
    p_send[:, :, half:] = lane_sq.astype(jnp.bfloat16)
    loads[3].wait()
    for j in range(0, half, step):
        term = fdot(hid[...], wd_oth[:, j : j + step])
        p_send[:, :, j : j + step] = term.astype(jnp.bfloat16).reshape(ep_count, seq, step)
    d_swap = remote(p_send, p_recv, d_sem.at[0], d_sem.at[1], me, other)
    d_swap.start()
    loads[4].wait()
    for j in range(0, half, step):
        p_own[:, :, j : j + step] = fdot(hid[...], wd_own[:, j : j + step]).reshape(
            ep_count, seq, step
        )
    d_swap.wait()

    def chip_sum(o):
        got = p_recv[o].astype(jnp.float32)
        return p_own[o] + got[:, :half], p_sq[o] + got[:, half:]

    plane_sends = {}
    for i in range(zn):
        dz = (i + 1) % zn
        for dq in range(1, pn):
            o = ((z + dz) % zn) * pn + (q + dq) % pn
            main, squares = chip_sum(o)
            s_send[o, :, :half] = main.astype(jnp.bfloat16)
            s_send[o, :, half:] = squares.astype(jnp.bfloat16)
            one = remote(
                s_send.at[o],
                r_recv.at[dq - 1, dz],
                rs_send.at[dz, dq],
                rs_recv.at[dz, dq],
                z * pn + (q + dq) % pn,
                c,
            )
            one.start()
            plane_sends[dz, dq] = one

    slots = ep_count * capp
    pick_from = lax.broadcasted_iota(jnp.int32, (full - width, slots), 0)
    pick_to = lax.broadcasted_iota(jnp.int32, (full - width, slots), 1) % capp
    pick = (pick_from == me * capp + pick_to).astype(jnp.float32).astype(jnp.bfloat16)
    chosen = fdot(gath[:, :, width:].reshape(rows_all, full - width), pick)
    row_owner = lax.broadcasted_iota(jnp.int32, (rows_all, slots), 0) // seq
    slot_owner = lax.broadcasted_iota(jnp.int32, (rows_all, slots), 1) // capp
    chosen = jnp.where(row_owner == slot_owner, chosen, 0.0).astype(jnp.bfloat16)
    for j in range(0, width, 512):
        rows[:, j : j + 512] = lax.dot_general(
            chosen,
            gath[:, :, j : j + 512].reshape(rows_all, 512),
            (((0,), (0,)), ((), ())),
            preferred_element_type=jnp.float32,
        ).astype(jnp.bfloat16)
    loads[5].wait()
    loads[6].wait()
    for j in range(0, xg.shape[1], step):
        act[:, j : j + step] = (
            silu(fdot(rows[...], xg[:, j : j + step])) * fdot(rows[...], xu[:, j : j + step])
        ).astype(jnp.bfloat16)
    loads[7].wait()
    for j in range(0, half, step):
        e_send[:, :, j : j + step] = (
            fdot(act[...], xd_oth[:, j : j + step])
            .reshape(ep_count, capp, step)
            .astype(jnp.bfloat16)
        )
    x_swap = remote(e_send, e_recv, x_sem.at[0], x_sem.at[1], me, other)
    x_swap.start()
    loads[8].wait()
    for j in range(0, half, step):
        e_own[:, :, j : j + step] = (
            fdot(act[...], xd_own[:, j : j + step])
            .reshape(ep_count, capp, step)
            .astype(jnp.bfloat16)
        )
    x_swap.wait()
    e_sum = (e_own[...].astype(jnp.float32) + e_recv[...].astype(jnp.float32)).astype(jnp.bfloat16)
    e_out[...] = e_sum
    e_ret[me] = e_out[me]
    backs = []
    for d in range(1, ep_count):
        peer = (me + d) % ep_count
        one = remote(e_out.at[peer], e_ret.at[me], er_send.at[d], er_recv.at[d], peer, c)
        one.start()
        backs.append(one)

    def plane_total(dz):
        main, squares = chip_sum(((z + dz) % zn) * pn + q)
        for dq in range(1, pn):
            plane_sends[dz, dq].wait_recv()
            got = r_recv[dq - 1, dz].astype(jnp.float32)
            main = main + got[:, :half]
            squares = squares + got[:, half:]
        return main, squares

    z_outs = []
    for dz in range(1, zn):
        main, squares = plane_total(dz)
        t_send[dz, :, :half] = main.astype(jnp.bfloat16)
        t_send[dz, :, half:] = squares.astype(jnp.bfloat16)
        one = remote(
            t_send.at[dz],
            z_recv.at[dz],
            zs_send.at[dz],
            zs_recv.at[dz],
            ((z + dz) % zn) * pn + q,
            c,
        )
        one.start()
        z_outs.append(one)
    main, squares = plane_total(0)
    for dz in range(1, zn):
        z_outs[dz - 1].wait_recv()
        got = z_recv[dz].astype(jnp.float32)
        main = main + got[:, :half]
        squares = squares + got[:, half:]
    inverse = lax.rsqrt(squares[:, :1] / ff2 + norm_eps)
    dense_out = (main * inverse).astype(jnp.bfloat16).astype(jnp.float32)
    for one in backs:
        one.wait_recv()
    returned = e_ret[...].reshape(slots, half)
    comb = comb_ref[...]
    comb_high = comb.astype(jnp.bfloat16)
    comb_low = (comb - comb_high.astype(jnp.float32)).astype(jnp.bfloat16)
    expert_sum = fdot(comb_high, returned) + fdot(comb_low, returned)
    res_ref[...] = (resid[:, own_cols] + expert_sum + branch * dense_out).astype(jnp.bfloat16)
    for one in plane_sends.values():
        one.wait_send()
    for one in z_outs:
        one.wait_send()
    for one in backs:
        one.wait_send()


def mlp_call(ep_count, capp, heads, tokens, gain, gate, place, comb, weights):
    zn = 2 ** ((ep_count.bit_length() - 1) // 2)
    pn = ep_count // zn
    seq, width = tokens.shape
    half = width // 2
    units = weights[1].shape[1]
    x_units = weights[4].shape[2]
    full = width + place.shape[1]
    slots = ep_count * capp
    lane = half + 128
    bf, f32 = jnp.bfloat16, jnp.float32
    dma = pltpu.SemaphoreType.DMA
    vm = pltpu.VMEM
    scratch = [
        vm(weights[0].shape, bf),
        vm((width, units), bf),
        vm((width, units), bf),
        vm((units, half), bf),
        vm((units, half), bf),
        vm((width, x_units), bf),
        vm((width, x_units), bf),
        vm((x_units, half), bf),
        vm((x_units, half), bf),
        vm((seq, width), bf),
        vm((seq, width), bf),
        vm((seq, width), f32),
        vm((ep_count, seq, full), bf),
        vm((ep_count * seq, units), bf),
        vm((ep_count, seq, half), f32),
        vm((ep_count, seq, 128), f32),
        vm((ep_count, seq, lane), bf),
        vm((ep_count, seq, lane), bf),
        vm((ep_count, seq, lane), bf),
        vm((pn - 1, zn, seq, lane), bf),
        vm((zn, seq, lane), bf),
        vm((zn, seq, lane), bf),
        vm((slots, width), bf),
        vm((slots, x_units), bf),
        vm((ep_count, capp, half), bf),
        vm((ep_count, capp, half), bf),
        vm((ep_count, capp, half), bf),
        vm((ep_count, capp, half), bf),
        vm((ep_count, capp, half), bf),
        dma((9,)),
        dma((2,)),
        dma((zn,)),
        dma((zn,)),
        dma((zn, pn)),
        dma((zn, pn)),
        dma((zn, pn)),
        dma((zn, pn)),
        dma((2,)),
        dma((zn, pn)),
        dma((zn, pn)),
        dma((zn,)),
        dma((zn,)),
        dma((2,)),
        dma((ep_count,)),
        dma((ep_count,)),
    ]
    return pl.pallas_call(
        functools.partial(mlp_kernel, ep_count, zn, capp, FF2),
        out_shape=jax.ShapeDtypeStruct((seq, half), bf),
        in_specs=[pl.BlockSpec(memory_space=pltpu.VMEM)] * 6
        + [pl.BlockSpec(memory_space=pl.ANY)] * 7,
        out_specs=pl.BlockSpec(memory_space=pltpu.VMEM),
        scratch_shapes=scratch,
        compiler_params=pltpu.CompilerParams(
            collective_id=0, has_side_effects=True, vmem_limit_bytes=60 * 1024 * 1024
        ),
    )(heads, tokens, gain, gate, place, comb, *weights)


def body(
    tokens,
    norm_gain,
    query_w,
    key_w,
    value_w,
    forget_w,
    forget_bias,
    query_gain,
    key_gain,
    cache_key,
    cache_value,
    cache_gate,
    cache_len,
    out_w,
    post_gain,
    branch_gate,
    dense_gate_w,
    dense_up_w,
    dense_down_w,
    expert_choice,
    route_weight,
    expert_gate_w,
    expert_up_w,
    expert_down_w,
):
    seq_count = tokens.shape[0]
    model_width = tokens.shape[1]
    heads_local = cache_gate.shape[1]
    kv_local = cache_key.shape[1]
    head_size = cache_key.shape[2]
    cache_span = cache_key.shape[3]
    tp_count = lax.axis_size("tp")
    ep_count = lax.axis_size("ep")
    tp_rank = lax.axis_index("tp")
    score_scale = head_size ** (-0.5)
    resid_in = tokens.astype(jnp.float32)
    normed = rms_scale(resid_in, norm_gain.astype(jnp.float32)).astype(jnp.bfloat16)
    queries = jnp.dot(normed, query_w, preferred_element_type=jnp.float32).reshape(
        seq_count, heads_local, head_size
    )
    queries = rms_scale(queries, query_gain.astype(jnp.float32)).astype(jnp.bfloat16)
    keys_all = jnp.dot(normed, key_w, preferred_element_type=jnp.float32).reshape(
        seq_count, -1, head_size
    )
    keys_all = rms_scale(keys_all, key_gain.astype(jnp.float32)).astype(jnp.bfloat16)
    values_all = (
        jnp.dot(normed, value_w, preferred_element_type=jnp.float32)
        .astype(jnp.bfloat16)
        .reshape(seq_count, -1, head_size)
    )
    fresh_key = lax.dynamic_slice_in_dim(keys_all, tp_rank * kv_local, kv_local, 1)
    fresh_value = lax.dynamic_slice_in_dim(values_all, tp_rank * kv_local, kv_local, 1)
    forget_all = jax.nn.log_sigmoid(
        jnp.dot(normed, forget_w, preferred_element_type=jnp.float32) + forget_bias
    )
    log_forget = lax.dynamic_slice_in_dim(forget_all, tp_rank * heads_local, heads_local, 1)
    repeat = heads_local // kv_local
    grouped = queries.reshape(seq_count, kv_local, repeat, head_size)
    scores = (
        jnp.einsum("sgrd,sgdl->sgrl", grouped, cache_key, preferred_element_type=jnp.float32)
        * score_scale
    )
    own_score = (
        jnp.einsum("sgrd,sgd->sgr", grouped, fresh_key, preferred_element_type=jnp.float32)
        * score_scale
    )
    current_slot_offset = lax.broadcasted_iota(jnp.int32, (seq_count, cache_span), 1)
    at_last = (current_slot_offset == cache_len[:, None] - 1)[:, None, :]
    previous = jnp.sum(jnp.where(at_last, cache_gate, jnp.zeros_like(cache_gate)), axis=2)
    current = previous + log_forget
    decay_bias = (current[:, :, None] - cache_gate).reshape(seq_count, kv_local, repeat, cache_span)
    is_valid = (current_slot_offset < cache_len[:, None])[:, None, None, :]
    logits = jnp.where(is_valid, scores + decay_bias, -jnp.inf)
    top_logit = jnp.maximum(jnp.max(logits, axis=3), own_score)
    weights = jnp.exp(logits - top_logit[..., None])
    own_weight = jnp.exp(own_score - top_logit)
    total_weight = jnp.sum(weights, axis=3) + own_weight
    cache_probs = (weights / total_weight[..., None]).astype(jnp.bfloat16)
    own_prob = (own_weight / total_weight).astype(jnp.bfloat16)
    mixed_heads = jnp.einsum(
        "sgrl,sgdl->sgrd", cache_probs, cache_value, preferred_element_type=jnp.float32
    )
    mixed_heads = (
        mixed_heads
        + own_prob.astype(jnp.float32)[..., None] * fresh_value.astype(jnp.float32)[:, :, None, :]
    )
    attn_heads = mixed_heads.reshape(seq_count, heads_local * head_size).astype(jnp.bfloat16)
    per_group = ep_count // GROUPS
    capacity = 2 * ((seq_count + 2 * per_group - 1) // (2 * per_group))
    capp = -(-capacity // 8) * 8
    route_count = expert_choice.shape[1]
    route_ids = expert_choice.reshape(-1)
    member = (route_ids[:, None] == jnp.arange(ep_count)[None, :]).astype(jnp.int32)
    slot_index = jnp.sum((jnp.cumsum(member, axis=0) - member) * member, axis=1)
    target = (route_ids * capp + slot_index).reshape(seq_count, route_count)
    slots = ep_count * capp
    place_width = -(-slots // 256) * 256
    hit = target[:, :, None] == jnp.arange(place_width)[None, None, :]
    place = jnp.any(hit, axis=1).astype(jnp.bfloat16)
    comb = jnp.sum(jnp.where(hit, route_weight[:, :, None], 0.0), axis=1)[:, :slots]
    mixed_out = mlp_call(
        ep_count,
        capp,
        attn_heads,
        tokens,
        post_gain.reshape(1, -1),
        branch_gate.reshape(1, -1),
        place,
        comb,
        (
            out_w,
            dense_gate_w,
            dense_up_w,
            dense_down_w,
            expert_gate_w,
            expert_up_w,
            expert_down_w,
        ),
    )
    return (mixed_out, fresh_key, fresh_value, current)


def solution(mesh):
    placed = (
        P("ep", None),
        P(),
        P(None, "tp"),
        P(),
        P(),
        P(),
        P(),
        P(),
        P(),
        P("ep", "tp", None, None),
        P("ep", "tp", None, None),
        P("ep", "tp", None),
        P("ep"),
        P("tp", None),
        P(),
        P(),
        P(None, ("ep", "tp")),
        P(None, ("ep", "tp")),
        P(("ep", "tp"), None),
        P("ep", None),
        P("ep", None),
        P("ep", None, "tp"),
        P("ep", None, "tp"),
        P("ep", "tp", None),
    )
    return jax.shard_map(
        body,
        mesh=mesh,
        in_specs=placed,
        out_specs=(P("ep", "tp"), P("ep", "tp", None), P("ep", "tp", None), P("ep", "tp")),
        check_vma=False,
    )
```

```python
import functools
import jax
import jax.numpy as jnp
from jax import lax
from jax.experimental import pallas as pl
from jax.experimental.pallas import tpu as pltpu
from jax.sharding import PartitionSpec as P

FF2 = 16384
GROUPS = 4


norm_eps = 1e-06


def rms_scale(values, gain_vec):
    mean_square = jnp.mean(values * values, axis=-1, keepdims=True)
    return values * lax.rsqrt(mean_square + norm_eps) * gain_vec


MESH = pl.DeviceIdType.MESH


def fdot(a, b):
    return jnp.dot(a, b, preferred_element_type=jnp.float32)


def silu(v):
    return v / (1.0 + jnp.exp(-v))


def mlp_kernel(
    ep_count,
    zn,
    capp,
    ff2,
    heads_ref,
    tok_ref,
    gain_ref,
    gate_ref,
    choice_ref,
    weight_ref,
    out_hbm,
    dg_hbm,
    du_hbm,
    dd_hbm,
    eg_hbm,
    eu_hbm,
    ed_hbm,
    res_ref,
    wout,
    wg,
    wu,
    wd_own,
    wd_oth,
    xg,
    xu,
    xd_own,
    xd_oth,
    part,
    part_in,
    resid,
    gath,
    hid,
    p_own,
    p_sq,
    p_send,
    p_recv,
    s_send,
    r_recv,
    t_send,
    z_recv,
    rows,
    act,
    e_own,
    e_send,
    e_recv,
    e_out,
    e_ret,
    wsem,
    tp_sem,
    a_send,
    a_recv,
    b_send,
    b_recv,
    f_send,
    f_recv,
    d_sem,
    rs_send,
    rs_recv,
    zs_send,
    zs_recv,
    x_sem,
    er_send,
    er_recv,
):
    pn = ep_count // zn
    me = lax.axis_index("ep")
    c = lax.axis_index("tp")
    z = me // pn
    q = me % pn
    other = 1 - c
    seq, width = tok_ref.shape
    half = width // 2
    full = gath.shape[2]
    fhalf = full // 2
    rows_all = ep_count * seq
    own_cols = pl.ds(pl.multiple_of(c * half, 128), half)
    oth_cols = pl.ds(pl.multiple_of(other * half, 128), half)
    g_cols = pl.ds(pl.multiple_of(c * fhalf, 128), fhalf)

    barrier = pltpu.get_barrier_semaphore()
    for d in range(1, ep_count):
        pl.semaphore_signal(
            barrier, inc=1, device_id=((me + d) % ep_count, c), device_id_type=MESH
        )
    pl.semaphore_signal(barrier, inc=1, device_id=(me, other), device_id_type=MESH)

    loads = [
        (out_hbm, wout),
        (dg_hbm, wg),
        (du_hbm, wu),
        (dd_hbm.at[:, oth_cols], wd_oth),
        (dd_hbm.at[:, own_cols], wd_own),
        (eg_hbm.at[0], xg),
        (eu_hbm.at[0], xu),
        (ed_hbm.at[0, :, oth_cols], xd_oth),
        (ed_hbm.at[0, :, own_cols], xd_own),
    ]
    loads = [pltpu.make_async_copy(a, b, wsem.at[i]) for i, (a, b) in enumerate(loads)]
    for one in loads:
        one.start()

    def remote(src, dst, ssem, rsem, ep_id, tp_id):
        return pltpu.make_async_remote_copy(
            src_ref=src,
            dst_ref=dst,
            send_sem=ssem,
            recv_sem=rsem,
            device_id=(ep_id, tp_id),
            device_id_type=MESH,
        )

    slots = ep_count * capp
    lanes = full - width
    lane_id = lax.broadcasted_iota(jnp.int32, (seq, lanes), 1)
    first = choice_ref[:, 0:1] == lane_id // capp
    second = choice_ref[:, 1:2] == lane_id // capp
    named = jnp.where(first, 1.0, jnp.where(second, 1.0, 0.0))
    earlier = lax.broadcasted_iota(jnp.int32, (seq, seq), 1) < lax.broadcasted_iota(
        jnp.int32, (seq, seq), 0
    )
    earlier = jnp.where(earlier, 1.0, 0.0).astype(jnp.bfloat16)
    rank = fdot(earlier, named.astype(jnp.bfloat16))
    hit = jnp.where(rank == (lane_id % capp).astype(jnp.float32), named, 0.0)
    comb = hit * jnp.where(first, weight_ref[:, 0:1], weight_ref[:, 1:2])
    gath[me, :, width:] = hit.astype(jnp.bfloat16)
    loads[0].wait()
    part[...] = fdot(heads_ref[...], wout[...]).astype(jnp.bfloat16)
    pl.semaphore_wait(barrier, ep_count)
    swap = remote(part, part_in, tp_sem.at[0], tp_sem.at[1], me, other)
    swap.start()
    swap.wait()
    attn = part[...].astype(jnp.float32) + part_in[...].astype(jnp.float32)
    res = (tok_ref[...].astype(jnp.float32) + attn).astype(jnp.bfloat16).astype(jnp.float32)
    resid[...] = res
    post = rms_scale(res, gain_ref[...].astype(jnp.float32)).astype(jnp.bfloat16)
    gath[me, :, :width] = post
    branch_in = jnp.sum(
        post.astype(jnp.float32) * gate_ref[...].astype(jnp.float32), axis=1, keepdims=True
    )
    branch = 1.0 / (1.0 + jnp.exp(-branch_in))

    sent = []

    def block_send(o, ssem, rsem, ep_id, tp_id):
        piece = gath.at[o, :, g_cols]
        one = remote(piece, piece, ssem, rsem, ep_id, tp_id)
        one.start()
        sent.append(one)
        return one

    z_sends = []
    for dz in range(1, zn):
        z_sends.append(
            block_send(me, a_send.at[dz], a_recv.at[dz], ((z + dz) % zn) * pn + q, c)
        )
    b_sends = {}
    f_sends = {}

    def to_plane(o, dz):
        for dq in range(1, pn):
            b_sends[dz, dq] = block_send(
                o, b_send.at[dz, dq], b_recv.at[dz, dq], z * pn + (q + dq) % pn, c
            )

    def to_partner(o, dz, dq):
        f_sends[dz, dq] = block_send(o, f_send.at[dz, dq], f_recv.at[dz, dq], me, other)

    units = wg.shape[1]
    step = min(256, units)
    group_rows = pn * seq

    def hidden_rows(dz):
        for dq in range(pn):
            if (dz, dq) in f_sends:
                f_sends[dz, dq].wait_recv()
        base = ((z + zn - dz) % zn) * pn
        blocks = pl.ds(base, pn)
        at_rows = pl.ds(pl.multiple_of(base * seq, group_rows), group_rows)
        x = gath[blocks, :, :width].reshape(group_rows, width)
        total_sq = jnp.zeros((group_rows, 1), jnp.float32)
        for j in range(0, units, step):
            h = silu(fdot(x, wg[:, j : j + step])) * fdot(x, wu[:, j : j + step])
            total_sq = total_sq + jnp.sum(h * h, axis=1, keepdims=True)
            hid[at_rows, j : j + step] = h.astype(jnp.bfloat16)
        lane_sq = jnp.broadcast_to(total_sq, (group_rows, 128)).reshape(pn, seq, 128)
        p_sq[blocks] = lane_sq
        p_send[blocks, :, half:] = lane_sq.astype(jnp.bfloat16)

    to_plane(me, 0)
    for dz in range(1, zn):
        z_sends[dz - 1].wait_recv()
        o = ((z + zn - dz) % zn) * pn + q
        to_plane(o, dz)
        to_partner(o, dz, 0)
    loads[1].wait()
    loads[2].wait()
    for dz in range(zn):
        for dq in range(1, pn):
            b_sends[dz, dq].wait_recv()
            o = ((z + zn - dz) % zn) * pn + (q + pn - dq) % pn
            to_partner(o, dz, dq)
        if dz > 0:
            hidden_rows(dz - 1)
    hidden_rows(zn - 1)
    for one in sent:
        one.wait_send()
    loads[3].wait()
    for j in range(0, half, step):
        term = fdot(hid[...], wd_oth[:, j : j + step])
        p_send[:, :, j : j + step] = term.astype(jnp.bfloat16).reshape(ep_count, seq, step)
    d_swap = remote(p_send, p_recv, d_sem.at[0], d_sem.at[1], me, other)
    d_swap.start()
    loads[4].wait()
    for j in range(0, half, step):
        p_own[:, :, j : j + step] = fdot(hid[...], wd_own[:, j : j + step]).reshape(
            ep_count, seq, step
        )
    d_swap.wait()

    def chip_sum(o):
        got = p_recv[o].astype(jnp.float32)
        return p_own[o] + got[:, :half], p_sq[o] + got[:, half:]

    plane_sends = {}
    for i in range(zn):
        dz = (i + 1) % zn
        for dq in range(1, pn):
            o = ((z + dz) % zn) * pn + (q + dq) % pn
            main, squares = chip_sum(o)
            s_send[o, :, :half] = main.astype(jnp.bfloat16)
            s_send[o, :, half:] = squares.astype(jnp.bfloat16)
            one = remote(
                s_send.at[o],
                r_recv.at[dq - 1, dz],
                rs_send.at[dz, dq],
                rs_recv.at[dz, dq],
                z * pn + (q + dq) % pn,
                c,
            )
            one.start()
            plane_sends[dz, dq] = one

    pick_from = lax.broadcasted_iota(jnp.int32, (full - width, slots), 0)
    pick_to = lax.broadcasted_iota(jnp.int32, (full - width, slots), 1) % capp
    pick = (pick_from == me * capp + pick_to).astype(jnp.float32).astype(jnp.bfloat16)
    chosen = fdot(gath[:, :, width:].reshape(rows_all, full - width), pick)
    row_owner = lax.broadcasted_iota(jnp.int32, (rows_all, slots), 0) // seq
    slot_owner = lax.broadcasted_iota(jnp.int32, (rows_all, slots), 1) // capp
    chosen = jnp.where(row_owner == slot_owner, chosen, 0.0).astype(jnp.bfloat16)
    for j in range(0, width, 512):
        rows[:, j : j + 512] = lax.dot_general(
            chosen,
            gath[:, :, j : j + 512].reshape(rows_all, 512),
            (((0,), (0,)), ((), ())),
            preferred_element_type=jnp.float32,
        ).astype(jnp.bfloat16)
    loads[5].wait()
    loads[6].wait()
    for j in range(0, xg.shape[1], step):
        act[:, j : j + step] = (
            silu(fdot(rows[...], xg[:, j : j + step])) * fdot(rows[...], xu[:, j : j + step])
        ).astype(jnp.bfloat16)
    loads[7].wait()
    for j in range(0, half, step):
        e_send[:, :, j : j + step] = (
            fdot(act[...], xd_oth[:, j : j + step])
            .reshape(ep_count, capp, step)
            .astype(jnp.bfloat16)
        )
    x_swap = remote(e_send, e_recv, x_sem.at[0], x_sem.at[1], me, other)
    x_swap.start()
    loads[8].wait()
    for j in range(0, half, step):
        e_own[:, :, j : j + step] = (
            fdot(act[...], xd_own[:, j : j + step])
            .reshape(ep_count, capp, step)
            .astype(jnp.bfloat16)
        )
    x_swap.wait()
    e_sum = (e_own[...].astype(jnp.float32) + e_recv[...].astype(jnp.float32)).astype(jnp.bfloat16)
    e_out[...] = e_sum
    e_ret[me] = e_out[me]
    backs = []
    for d in range(1, ep_count):
        peer = (me + d) % ep_count
        one = remote(e_out.at[peer], e_ret.at[me], er_send.at[d], er_recv.at[d], peer, c)
        one.start()
        backs.append(one)

    def plane_total(dz):
        main, squares = chip_sum(((z + dz) % zn) * pn + q)
        for dq in range(1, pn):
            plane_sends[dz, dq].wait_recv()
            got = r_recv[dq - 1, dz].astype(jnp.float32)
            main = main + got[:, :half]
            squares = squares + got[:, half:]
        return main, squares

    z_outs = []
    for dz in range(1, zn):
        main, squares = plane_total(dz)
        t_send[dz, :, :half] = main.astype(jnp.bfloat16)
        t_send[dz, :, half:] = squares.astype(jnp.bfloat16)
        one = remote(
            t_send.at[dz],
            z_recv.at[dz],
            zs_send.at[dz],
            zs_recv.at[dz],
            ((z + dz) % zn) * pn + q,
            c,
        )
        one.start()
        z_outs.append(one)
    main, squares = plane_total(0)
    for dz in range(1, zn):
        z_outs[dz - 1].wait_recv()
        got = z_recv[dz].astype(jnp.float32)
        main = main + got[:, :half]
        squares = squares + got[:, half:]
    inverse = lax.rsqrt(squares[:, :1] / ff2 + norm_eps)
    dense_out = (main * inverse).astype(jnp.bfloat16).astype(jnp.float32)
    for one in backs:
        one.wait_recv()
    returned = e_ret[...].reshape(slots, half)
    comb = comb[:, :slots]
    comb_high = comb.astype(jnp.bfloat16)
    comb_low = (comb - comb_high.astype(jnp.float32)).astype(jnp.bfloat16)
    expert_sum = fdot(comb_high, returned) + fdot(comb_low, returned)
    res_ref[...] = (resid[:, own_cols] + expert_sum + branch * dense_out).astype(jnp.bfloat16)
    for one in plane_sends.values():
        one.wait_send()
    for one in z_outs:
        one.wait_send()
    for one in backs:
        one.wait_send()


def mlp_call(ep_count, capp, heads, tokens, gain, gate, choice, route_weight, weights):
    zn = 2 ** ((ep_count.bit_length() - 1) // 2)
    pn = ep_count // zn
    seq, width = tokens.shape
    half = width // 2
    units = weights[1].shape[1]
    x_units = weights[4].shape[2]
    slots = ep_count * capp
    full = width - (-slots // 256) * 256
    lane = half + 128
    bf, f32 = jnp.bfloat16, jnp.float32
    dma = pltpu.SemaphoreType.DMA
    vm = pltpu.VMEM
    scratch = [
        vm(weights[0].shape, bf),
        vm((width, units), bf),
        vm((width, units), bf),
        vm((units, half), bf),
        vm((units, half), bf),
        vm((width, x_units), bf),
        vm((width, x_units), bf),
        vm((x_units, half), bf),
        vm((x_units, half), bf),
        vm((seq, width), bf),
        vm((seq, width), bf),
        vm((seq, width), f32),
        vm((ep_count, seq, full), bf),
        vm((ep_count * seq, units), bf),
        vm((ep_count, seq, half), f32),
        vm((ep_count, seq, 128), f32),
        vm((ep_count, seq, lane), bf),
        vm((ep_count, seq, lane), bf),
        vm((ep_count, seq, lane), bf),
        vm((pn - 1, zn, seq, lane), bf),
        vm((zn, seq, lane), bf),
        vm((zn, seq, lane), bf),
        vm((slots, width), bf),
        vm((slots, x_units), bf),
        vm((ep_count, capp, half), bf),
        vm((ep_count, capp, half), bf),
        vm((ep_count, capp, half), bf),
        vm((ep_count, capp, half), bf),
        vm((ep_count, capp, half), bf),
        dma((9,)),
        dma((2,)),
        dma((zn,)),
        dma((zn,)),
        dma((zn, pn)),
        dma((zn, pn)),
        dma((zn, pn)),
        dma((zn, pn)),
        dma((2,)),
        dma((zn, pn)),
        dma((zn, pn)),
        dma((zn,)),
        dma((zn,)),
        dma((2,)),
        dma((ep_count,)),
        dma((ep_count,)),
    ]
    return pl.pallas_call(
        functools.partial(mlp_kernel, ep_count, zn, capp, FF2),
        out_shape=jax.ShapeDtypeStruct((seq, half), bf),
        in_specs=[pl.BlockSpec(memory_space=pltpu.VMEM)] * 6
        + [pl.BlockSpec(memory_space=pl.ANY)] * 7,
        out_specs=pl.BlockSpec(memory_space=pltpu.VMEM),
        scratch_shapes=scratch,
        compiler_params=pltpu.CompilerParams(
            collective_id=0, has_side_effects=True, vmem_limit_bytes=60 * 1024 * 1024
        ),
    )(heads, tokens, gain, gate, choice, route_weight, *weights)


def body(
    tokens,
    norm_gain,
    query_w,
    key_w,
    value_w,
    forget_w,
    forget_bias,
    query_gain,
    key_gain,
    cache_key,
    cache_value,
    cache_gate,
    cache_len,
    out_w,
    post_gain,
    branch_gate,
    dense_gate_w,
    dense_up_w,
    dense_down_w,
    expert_choice,
    route_weight,
    expert_gate_w,
    expert_up_w,
    expert_down_w,
):
    seq_count = tokens.shape[0]
    model_width = tokens.shape[1]
    heads_local = cache_gate.shape[1]
    kv_local = cache_key.shape[1]
    head_size = cache_key.shape[2]
    cache_span = cache_key.shape[3]
    tp_count = lax.axis_size("tp")
    ep_count = lax.axis_size("ep")
    tp_rank = lax.axis_index("tp")
    score_scale = head_size ** (-0.5)
    resid_in = tokens.astype(jnp.float32)
    normed = rms_scale(resid_in, norm_gain.astype(jnp.float32)).astype(jnp.bfloat16)
    queries = jnp.dot(normed, query_w, preferred_element_type=jnp.float32).reshape(
        seq_count, heads_local, head_size
    )
    queries = rms_scale(queries, query_gain.astype(jnp.float32)).astype(jnp.bfloat16)
    keys_all = jnp.dot(normed, key_w, preferred_element_type=jnp.float32).reshape(
        seq_count, -1, head_size
    )
    keys_all = rms_scale(keys_all, key_gain.astype(jnp.float32)).astype(jnp.bfloat16)
    values_all = (
        jnp.dot(normed, value_w, preferred_element_type=jnp.float32)
        .astype(jnp.bfloat16)
        .reshape(seq_count, -1, head_size)
    )
    fresh_key = lax.dynamic_slice_in_dim(keys_all, tp_rank * kv_local, kv_local, 1)
    fresh_value = lax.dynamic_slice_in_dim(values_all, tp_rank * kv_local, kv_local, 1)
    forget_all = jax.nn.log_sigmoid(
        jnp.dot(normed, forget_w, preferred_element_type=jnp.float32) + forget_bias
    )
    log_forget = lax.dynamic_slice_in_dim(forget_all, tp_rank * heads_local, heads_local, 1)
    repeat = heads_local // kv_local
    grouped = queries.reshape(seq_count, kv_local, repeat, head_size)
    scores = (
        jnp.einsum("sgrd,sgdl->sgrl", grouped, cache_key, preferred_element_type=jnp.float32)
        * score_scale
    )
    own_score = (
        jnp.einsum("sgrd,sgd->sgr", grouped, fresh_key, preferred_element_type=jnp.float32)
        * score_scale
    )
    current_slot_offset = lax.broadcasted_iota(jnp.int32, (seq_count, cache_span), 1)
    at_last = (current_slot_offset == cache_len[:, None] - 1)[:, None, :]
    previous = jnp.sum(jnp.where(at_last, cache_gate, jnp.zeros_like(cache_gate)), axis=2)
    current = previous + log_forget
    decay_bias = (current[:, :, None] - cache_gate).reshape(seq_count, kv_local, repeat, cache_span)
    is_valid = (current_slot_offset < cache_len[:, None])[:, None, None, :]
    logits = jnp.where(is_valid, scores + decay_bias, -jnp.inf)
    top_logit = jnp.maximum(jnp.max(logits, axis=3), own_score)
    weights = jnp.exp(logits - top_logit[..., None])
    own_weight = jnp.exp(own_score - top_logit)
    total_weight = jnp.sum(weights, axis=3) + own_weight
    cache_probs = (weights / total_weight[..., None]).astype(jnp.bfloat16)
    own_prob = (own_weight / total_weight).astype(jnp.bfloat16)
    mixed_heads = jnp.einsum(
        "sgrl,sgdl->sgrd", cache_probs, cache_value, preferred_element_type=jnp.float32
    )
    mixed_heads = (
        mixed_heads
        + own_prob.astype(jnp.float32)[..., None] * fresh_value.astype(jnp.float32)[:, :, None, :]
    )
    attn_heads = mixed_heads.reshape(seq_count, heads_local * head_size).astype(jnp.bfloat16)
    per_group = ep_count // GROUPS
    capacity = 2 * ((seq_count + 2 * per_group - 1) // (2 * per_group))
    capp = -(-capacity // 8) * 8
    mixed_out = mlp_call(
        ep_count,
        capp,
        attn_heads,
        tokens,
        post_gain.reshape(1, -1),
        branch_gate.reshape(1, -1),
        expert_choice,
        route_weight,
        (
            out_w,
            dense_gate_w,
            dense_up_w,
            dense_down_w,
            expert_gate_w,
            expert_up_w,
            expert_down_w,
        ),
    )
    return (mixed_out, fresh_key, fresh_value, current)


def solution(mesh):
    placed = (
        P("ep", None),
        P(),
        P(None, "tp"),
        P(),
        P(),
        P(),
        P(),
        P(),
        P(),
        P("ep", "tp", None, None),
        P("ep", "tp", None, None),
        P("ep", "tp", None),
        P("ep"),
        P("tp", None),
        P(),
        P(),
        P(None, ("ep", "tp")),
        P(None, ("ep", "tp")),
        P(("ep", "tp"), None),
        P("ep", None),
        P("ep", None),
        P("ep", None, "tp"),
        P("ep", None, "tp"),
        P("ep", "tp", None),
    )
    return jax.shard_map(
        body,
        mesh=mesh,
        in_specs=placed,
        out_specs=(P("ep", "tp"), P("ep", "tp", None), P("ep", "tp", None), P("ep", "tp")),
        check_vma=False,
    )
```
